32 devices in a mesh: rep: 4 (over z), fs: 2 (over y), tp: 4 (over x, core).
Axes of the slice: x: 2, y: 2, z: 4, core: 2. Of those that a mesh axis runs over, the one named last changes fastest.
Arguments:
- layer_input: bfloat16 [3072, 2048], P('rep', ('fs', 'tp')), may hold values from -0.8046875 to 0.8046875
- gate_saved: bfloat16 [3072, 5120], P('rep', 'tp'), may hold values from -6 to 6
- up_saved: bfloat16 [3072, 5120], P('rep', 'tp'), may hold values from -6 to 6
- out_grad: bfloat16 [3072, 2048], P('rep'), may hold values from -0.8046875 to 0.8046875
- conv_taps: bfloat16 [3, 5120], P(None, 'tp'), may hold values from -3.5 to 3.5
- w_gate: bfloat16 [2048, 5120], P('fs', 'tp'), may hold values from -0.125 to 0.125
- w_up: bfloat16 [2048, 5120], P('fs', 'tp'), may hold values from -0.125 to 0.125
- w_down: bfloat16 [5120, 2048], P('tp', 'fs'), may hold values from -0.078125 to 0.078125
Outputs:
- input_grad: bfloat16 [3072, 2048], P('rep', ('fs', 'tp'))
- gate_grad: float32 [2048, 5120], P('fs', 'tp')
- up_grad: float32 [2048, 5120], P('fs', 'tp')
- down_grad: float32 [5120, 2048], P('tp', 'fs')
- taps_grad: float32 [3, 5120], P(None, 'tp')
The draws below stay inside these ranges and needn't reach their ends.
All inputs are finite; a program needn't handle non-finite values.
Results may differ from the reference program's by a relative error of at most 0.018.
Values may be sent and summed in bfloat16 or wider, within the bound.
A program may use at most 128 MiB of HBM per device.

```python
import jax
import jax.numpy as jnp
from jax import lax

D = 2048
FF = 5120
TAPS = 3
TOK_DEV = 768
TOKENS = 3072
HID_TP = 1280
N_TP = 4


def spiked(array, stream_key, source, target, shards_of, factor):
    def block_of(position):
        return (jnp.arange(array.shape[position]) // (array.shape[position] // shards_of)).reshape((-1,) + (1,) * (array.ndim - 1 - position))

    one_side = jax.random.permutation(stream_key, shards_of)[block_of(target)]
    second = (block_of(target) + shards_of // 2) % shards_of
    return jnp.where((block_of(source) == one_side) | (block_of(source) == second), factor * array, array)


def level_of(key, shape, cuts, smallest, largest):
    loudness = 1.0
    for dim, shards_of in cuts:
        steps = jax.random.uniform(jax.random.fold_in(jax.random.fold_in(key, 6), dim), (shards_of,), jnp.float32, smallest / len(cuts), largest / len(cuts))
        loudness = loudness * jnp.repeat(jnp.exp(steps), shape[dim] // shards_of).reshape((-1,) + (1,) * (len(shape) - 1 - dim))
    return loudness


def bell_draw(own_key, dims, width, most, cuts=(), held_as=jnp.bfloat16):
    level = level_of(own_key, dims, cuts, -0.22, 0.18) if cuts else 1.0
    values = jax.random.normal(own_key, dims, jnp.float32) * width * level
    return jnp.minimum(jnp.maximum(values, -most), most).astype(held_as)


def heavy_noise(key, shape, scale, bound, split, heavy, dtype=jnp.bfloat16):
    drawn = scale * jax.random.normal(key, shape, jnp.float32)
    if split:
        drawn = drawn * level_of(key, shape, split, -0.22, 0.18)
    return jnp.clip(spiked(drawn, jax.random.fold_in(key, 3), *heavy), -bound, bound).astype(dtype)


def setup_inputs(seed: int = 0) -> dict:
    key_list = jax.random.split(jax.random.key(seed), 9)
    layer_input = bell_draw(key_list[0], (TOKENS, D), (TOKENS ** -0.25), 0.8046875, ((0, 4), (1, 8)))
    gate_saved = bell_draw(key_list[1], (TOKENS, FF), 1.0, 6.0, ((0, 4), (1, 4)))
    up_saved = bell_draw(key_list[2], (TOKENS, FF), 1.0, 6.0, ((0, 4), (1, 4)))
    out_grad = heavy_noise(key_list[3], (TOKENS, D), (TOKENS ** -0.25), 0.8046875, ((0, 4),), (0, 1, 4, 2.0))
    conv_taps = bell_draw(key_list[4], (TAPS, FF), TAPS ** -0.5, 3.5, ((1, 4),))
    w_gate = bell_draw(key_list[5], (D, FF), D ** -0.5, 0.125, ((0, 2), (1, 4)))
    w_up = bell_draw(key_list[6], (D, FF), D ** -0.5, 0.125, ((0, 2), (1, 4)))
    w_down = bell_draw(key_list[7], (FF, D), FF ** -0.5, 0.078125, ((0, 4), (1, 2)))
    return {"layer_input": layer_input, "gate_saved": gate_saved, "up_saved": up_saved, "out_grad": out_grad, "conv_taps": conv_taps, "w_gate": w_gate, "w_up": w_up, "w_down": w_down}


def shift_back(values, count):
    padded = jnp.pad(values, ((0, 0), (count, 0), (0, 0)))
    return padded[:, :TOK_DEV]


def shift_ahead(values, count):
    padded = jnp.pad(values, ((0, 0), (0, count), (0, 0)))
    return padded[:, count:]


def reference(layer_input, gate_saved, up_saved, out_grad, conv_taps, w_gate, w_up, w_down):
    act_grad = jnp.dot(out_grad, w_down.T, preferred_element_type=jnp.float32)
    seq_count = TOKENS // TOK_DEV
    gate_float = gate_saved.astype(jnp.float32).reshape(seq_count, TOK_DEV, FF)
    up_float = up_saved.astype(jnp.float32).reshape(seq_count, TOK_DEV, FF)
    grad_float = act_grad.reshape(seq_count, TOK_DEV, FF)
    taps_float = conv_taps.astype(jnp.float32)
    back_one = shift_back(gate_float, 1)
    back_two = shift_back(gate_float, 2)
    conv_out = taps_float[0] * back_two + taps_float[1] * back_one + taps_float[2] * gate_float
    gate_sig = jax.nn.sigmoid(conv_out)
    swish_out = conv_out * gate_sig
    activation = (swish_out * up_float).astype(jnp.bfloat16).reshape(TOKENS, FF)
    up_part = (grad_float * swish_out).astype(jnp.bfloat16).reshape(TOKENS, FF)
    conv_grad = grad_float * up_float * gate_sig * (1.0 + conv_out * (1.0 - gate_sig))
    ahead_one = shift_ahead(conv_grad, 1)
    ahead_two = shift_ahead(conv_grad, 2)
    gate_part = (taps_float[0] * ahead_two + taps_float[1] * ahead_one + taps_float[2] * conv_grad)
    gate_part = gate_part.astype(jnp.bfloat16).reshape(TOKENS, FF)
    taps_grad = jnp.stack([jnp.sum(conv_grad * back_two, axis=(0, 1)),
                           jnp.sum(conv_grad * back_one, axis=(0, 1)),
                           jnp.sum(conv_grad * gate_float, axis=(0, 1))])
    down_grad = jnp.dot(activation.T, out_grad, preferred_element_type=jnp.float32)
    gate_grad = jnp.dot(layer_input.T, gate_part, preferred_element_type=jnp.float32)
    up_grad = jnp.dot(layer_input.T, up_part, preferred_element_type=jnp.float32)
    gate_blocks = gate_part.astype(jnp.float32).reshape(TOKENS, N_TP, HID_TP)
    up_blocks = up_part.astype(jnp.float32).reshape(TOKENS, N_TP, HID_TP)
    wgate_blocks = w_gate.astype(jnp.float32).reshape(D, N_TP, HID_TP)
    wup_blocks = w_up.astype(jnp.float32).reshape(D, N_TP, HID_TP)
    block_term = jnp.einsum('thf,dhf->htd', gate_blocks, wgate_blocks) + jnp.einsum('thf,dhf->htd', up_blocks, wup_blocks)
    block_term = lax.optimization_barrier(block_term.astype(jnp.bfloat16))
    input_grad = jnp.sum(block_term.astype(jnp.float32), axis=0).astype(jnp.bfloat16)
    return (input_grad, gate_grad, up_grad, down_grad, taps_grad)
```

```python
import functools

import jax
import jax.numpy as jnp
from jax import lax
from jax.experimental import pallas as pl
from jax.experimental.pallas import tpu as pltpu
from jax.sharding import PartitionSpec as P

MESH = pl.DeviceIdType.MESH
F32 = jnp.float32
BF16 = jnp.bfloat16
CH = 128
HALF = CH // 2


def kernel(n_rep, n_fs, n_tp, x_in, gate_in, up_in, og_in, taps_in, wg_in, wu_in, wd_in,
           from_in, ig_out, taps_out,
           xb, gate, up, og, wg, wu, wd, part, from_out, gp, upp, terms, terms_in, taps_all,
           xs_sem, xr_sem, gl_sem, ul_sem, ld_sem, wl_sem, ws_sem, wr_sem,
           in_s, in_r, out_s, out_r, ts_sem, tr_sem, ps_sem, pr_sem):
    rep, fs, tp = lax.axis_index("rep"), lax.axis_index("fs"), lax.axis_index("tp")
    seq, hid = gate.shape
    dw = wd_in.shape[1]
    w = x_in.shape[1]
    nj = hid // CH
    half = n_rep // 2
    low = rep < half
    depth = jnp.where(low, rep, n_rep - 1 - rep)
    inward = jnp.where(low, rep + 1, rep - 1)
    outward = jnp.where(low, rep - 1, rep + 1)
    has_out = depth > 0
    outward = jnp.where(has_out, outward, inward)
    innermost = depth == half - 1
    lag = 2 + 18 * (half - 1 - depth)
    lead = min(4, nj)
    steps = 3 * nj

    def rows(j):
        return pl.ds(pl.multiple_of(j * CH, CH), CH)

    def piece(i):
        return pl.ds(pl.multiple_of(i * HALF, HALF), HALF)

    def unit(i):
        v, h = lax.div(i, 2), lax.rem(i, 2)
        a = v - lead
        b = a - 3 * (nj - lead)
        m = lax.rem(a, 3)
        mid = a < 3 * (nj - lead)
        first = a < 0
        k = jnp.where(first, 0, jnp.where(mid, jnp.where(m == 2, 0, m + 1), 1 + lax.rem(b, 2)))
        j = jnp.where(first, v, jnp.where(
            mid, lax.div(a, 3) + jnp.where(m == 2, lead, 0), nj - lead + lax.div(b, 2)))
        return 2 * j + h, k

    def fs_peer(d):
        return lax.rem(fs + d, n_fs)

    def tp_peer(d):
        return lax.rem(tp + d, n_tp)

    def load_gate(j):
        return pltpu.make_async_copy(gate_in.at[:, rows(j)], gate.at[:, rows(j)], gl_sem.at[j])

    def load_up(j):
        return pltpu.make_async_copy(up_in.at[:, rows(j)], up.at[:, rows(j)], ul_sem.at[j])

    def load_wd(j):
        return pltpu.make_async_copy(wd_in.at[rows(j), :], wd.at[fs, rows(j), :], wl_sem.at[j])

    def send_wd(j, d):
        return pltpu.make_async_remote_copy(
            src_ref=wd_in.at[rows(j), :], dst_ref=wd.at[fs, rows(j), :],
            send_sem=ws_sem.at[d - 1, j], recv_sem=wr_sem.at[d - 1, j],
            device_id={"fs": fs_peer(d)}, device_id_type=MESH)

    def recv_wd(j, d):
        src = lax.rem(fs + n_fs - d, n_fs)
        return pltpu.make_async_remote_copy(
            src_ref=wd_in.at[rows(j), :], dst_ref=wd.at[src, rows(j), :],
            send_sem=ws_sem.at[d - 1, j], recv_sem=wr_sem.at[d - 1, j],
            device_id={"fs": fs_peer(d)}, device_id_type=MESH)

    def x_copy(d, slot):
        return pltpu.make_async_remote_copy(
            src_ref=x_in, dst_ref=xb.at[slot], send_sem=xs_sem.at[d - 1], recv_sem=xr_sem.at[d - 1],
            device_id={"tp": tp_peer(d)}, device_id_type=MESH)

    def term_copy(d):
        return pltpu.make_async_remote_copy(
            src_ref=terms.at[tp_peer(d)], dst_ref=terms_in.at[d - 1],
            send_sem=ts_sem.at[d - 1], recv_sem=tr_sem.at[d - 1],
            device_id={"tp": tp_peer(d)}, device_id_type=MESH)

    def taps_copy(d, slot):
        return pltpu.make_async_remote_copy(
            src_ref=taps_all.at[rep], dst_ref=taps_all.at[slot],
            send_sem=ps_sem.at[d - 1], recv_sem=pr_sem.at[d - 1],
            device_id={"rep": lax.rem(rep + d, n_rep)}, device_id_type=MESH)

    def in_copy(j, k, dst):
        return pltpu.make_async_remote_copy(
            src_ref=part.at[k, piece(j), :], dst_ref=dst.at[k, piece(j), :],
            send_sem=in_s.at[k, j], recv_sem=(in_r if dst is from_out else out_r).at[k, j],
            device_id={"rep": inward}, device_id_type=MESH)

    def out_copy(j, k):
        return pltpu.make_async_remote_copy(
            src_ref=from_in.at[k, piece(j), :], dst_ref=from_in.at[k, piece(j), :],
            send_sem=out_s.at[k, j], recv_sem=out_r.at[k, j],
            device_id={"rep": outward}, device_id_type=MESH)

    loads = [
        pltpu.make_async_copy(og_in, og, ld_sem.at[0]),
        pltpu.make_async_copy(wg_in, wg, ld_sem.at[1]),
        pltpu.make_async_copy(wu_in, wu, ld_sem.at[2]),
        pltpu.make_async_copy(x_in, xb.at[tp], ld_sem.at[3]),
    ]
    load_gate(0).start()
    load_up(0).start()
    loads[0].start()
    load_wd(0).start()
    loads[3].start()

    barrier = pltpu.get_barrier_semaphore()
    for axis, n, me in (("rep", n_rep, rep), ("fs", n_fs, fs), ("tp", n_tp, tp)):
        for d in range(1, n):
            pl.semaphore_signal(barrier, inc=1, device_id={axis: lax.rem(me + d, n)}, device_id_type=MESH)
    pl.semaphore_wait(barrier, n_rep + n_fs + n_tp - 3)

    for d in range(1, n_tp):
        x_copy(d, tp).start()

    def send_all(j, c):
        for d in range(1, n_fs):
            send_wd(j, d).start()
        return c
    lax.fori_loop(0, nj, send_all, 0)

    def load_rest(j, c):
        load_gate(j).start()
        load_up(j).start()
        load_wd(j).start()
        return c
    lax.fori_loop(1, nj, load_rest, 0)
    loads[1].start()
    loads[2].start()

    pos = lax.broadcasted_iota(jnp.int32, (seq, CH), 0)

    def back(v, n):
        return jnp.where(pos >= n, pltpu.roll(v, n, 0), 0.0)

    def ahead(v, n):
        return jnp.where(pos < seq - n, pltpu.roll(v, seq - n, 0), 0.0)

    def conv(j):
        g = gate[:, rows(j)].astype(F32)
        t = taps_in[:, rows(j)].astype(F32)
        b1, b2 = back(g, 1), back(g, 2)
        return g, b1, b2, t, t[0:1] * b2 + t[1:2] * b1 + t[2:3] * g

    tdot = functools.partial(lax.dot_general, dimension_numbers=(((0,), (0,)), ((), ())),
                             preferred_element_type=F32)
    wdot = functools.partial(lax.dot_general, dimension_numbers=(((1,), (1,)), ((), ())),
                             preferred_element_type=F32)

    def compute_down(j):
        load_gate(j).wait()
        load_up(j).wait()
        g, b1, b2, t, co = conv(j)
        act = (co * jax.nn.sigmoid(co) * up[:, rows(j)].astype(F32)).astype(BF16)
        cols = pl.ds(pl.multiple_of(fs * dw, dw), dw)
        part[0, rows(j), :] = tdot(act, og[:, cols]).astype(BF16)

    def compute_rest(j):
        load_wd(j).wait()
        for d in range(1, n_fs):
            recv_wd(j, d).wait_recv()
        ag = wdot(og[:, 0:dw], wd[0, rows(j), :])
        for f in range(1, n_fs):
            ag = ag + wdot(og[:, f * dw:(f + 1) * dw], wd[f, rows(j), :])
        g, b1, b2, t, co = conv(j)
        s = jax.nn.sigmoid(co)
        u_part = (ag * (co * s)).astype(BF16)
        cg = ag * up[:, rows(j)].astype(F32) * s * (1.0 + co * (1.0 - s))
        g_part = (t[0:1] * ahead(cg, 2) + t[1:2] * ahead(cg, 1) + t[2:3] * cg).astype(BF16)
        taps_all[rep, 0:1, rows(j)] = jnp.sum(cg * b2, axis=0, keepdims=True)
        taps_all[rep, 1:2, rows(j)] = jnp.sum(cg * b1, axis=0, keepdims=True)
        taps_all[rep, 2:3, rows(j)] = jnp.sum(cg * g, axis=0, keepdims=True)
        gp[:, rows(j)] = g_part
        upp[:, rows(j)] = u_part

        @pl.when(j == 0)
        def _():
            loads[3].wait()
            for d in range(1, n_tp):
                x_copy(d, lax.rem(tp + n_tp - d, n_tp)).wait_recv()
        for b in range(n_tp):
            part[1, rows(j), b * w:(b + 1) * w] = tdot(g_part, xb[b]).astype(BF16)
            part[2, rows(j), b * w:(b + 1) * w] = tdot(u_part, xb[b]).astype(BF16)

    def compute_term(d):
        @pl.when(d == 1)
        def _():
            for p in range(1, n_rep):
                taps_copy(p, rep).start()
            loads[1].wait()
            loads[2].wait()
        b = tp_peer(d)
        r = pl.ds(pl.multiple_of(b * w, w), w)
        terms[b] = (wdot(gp[...], wg[r, :]) + wdot(upp[...], wu[r, :])).astype(BF16)

        @pl.when(d < n_tp)
        def _():
            term_copy(d).start()

    def q_stage(j, k):
        @pl.when(has_out)
        def _():
            in_copy(j, k, from_out).wait_recv()
            r = piece(j)
            part[k, r, :] = (part[k, r, :].astype(F32) + from_out[k, r, :].astype(F32)).astype(BF16)

        @pl.when(innermost)
        def _():
            in_copy(j, k, from_in).start()

        @pl.when(jnp.logical_not(innermost))
        def _():
            in_copy(j, k, from_out).start()

    def s_stage(j, k):
        out_copy(j, k).wait_recv()

        @pl.when(innermost)
        def _():
            r = piece(j)
            from_in[k, r, :] = (part[k, r, :].astype(F32) + from_in[k, r, :].astype(F32)).astype(BF16)

        @pl.when(has_out)
        def _():
            out_copy(j, k).start()

    loads[0].wait()
    compute_down(0)

    def step(v, c):
        for h in range(2):
            i = 2 * v + h

            @pl.when(v < steps)
            def _():
                q_stage(*unit(i))
            si = i - lag

            @pl.when(jnp.logical_and(si >= 0, si < 2 * steps))
            def _():
                s_stage(*unit(si))
        a = v - (lead - 1)
        b = a - 2 * (nj - lead)
        early = a < 0
        mid = jnp.logical_and(a >= 0, b < 0)
        is_down = jnp.logical_or(early, jnp.logical_and(mid, lax.rem(a, 2) == 1))
        is_rest = jnp.logical_and(jnp.logical_not(is_down), b < lead)

        @pl.when(is_down)
        def _():
            compute_down(jnp.where(early, v + 1, lead + lax.div(a, 2)))

        @pl.when(is_rest)
        def _():
            compute_rest(jnp.where(mid, lax.div(a, 2), nj - lead + b))

        @pl.when(jnp.logical_and(b >= lead, b < lead + n_tp))
        def _():
            compute_term(b - lead + 1)
        return c
    lax.fori_loop(0, steps + (2 + 1) // 2 + 9 * (half - 1), step, 0)

    total = terms[tp].astype(F32)
    for d in range(1, n_tp):
        term_copy(d).wait_recv()
        total = total + terms_in[d - 1].astype(F32)
    ig_out[...] = total.astype(BF16)
    for d in range(1, n_rep):
        taps_copy(d, lax.rem(rep + n_rep - d, n_rep)).wait_recv()
    acc = taps_all[0]
    for i in range(1, n_rep):
        acc = acc + taps_all[i]
    taps_out[...] = acc

    for d in range(1, n_tp):
        x_copy(d, tp).wait_send()
        term_copy(d).wait_send()
    for d in range(1, n_rep):
        taps_copy(d, rep).wait_send()

    def drain(j, c):
        for d in range(1, n_fs):
            send_wd(j, d).wait_send()
        for k in range(3):
            for i in (2 * j, 2 * j + 1):
                in_copy(i, k, from_out).wait_send()

                @pl.when(has_out)
                def _():
                    out_copy(i, k).wait_send()
        return c
    lax.fori_loop(0, nj, drain, 0)


def widen(grads, input_grad, taps, ig_out, gate_out, up_out, down_out, taps_out):
    down_out[...] = grads[0].astype(F32)
    gate_out[...] = grads[1].astype(F32).T
    up_out[...] = grads[2].astype(F32).T

    @pl.when(pl.program_id(0) == 0)
    def _():
        ig_out[...] = input_grad[...]
        taps_out[...] = taps[0:3, :]


def solution(mesh):
    n_rep, n_fs, n_tp = mesh.shape["rep"], mesh.shape["fs"], mesh.shape["tp"]

    def local(layer_input, gate_saved, up_saved, out_grad, conv_taps, w_gate, w_up, w_down):
        seq, w = layer_input.shape
        dw, hid = w_gate.shape
        width = out_grad.shape[1]
        nj = hid // CH
        any_spec = pl.BlockSpec(memory_space=pl.ANY)
        vmem = pl.BlockSpec(memory_space=pltpu.VMEM)
        dma = pltpu.SemaphoreType.DMA
        grads, input_grad, taps = pl.pallas_call(
            functools.partial(kernel, n_rep, n_fs, n_tp),
            out_shape=(
                pltpu.VMEM((3, hid, dw), BF16),
                pltpu.VMEM((seq, w), BF16),
                pltpu.VMEM((8, hid), F32),
            ),
            in_specs=[any_spec] * 4 + [vmem] + [any_spec] * 3,
            out_specs=(vmem, vmem, vmem),
            scratch_shapes=[
                pltpu.VMEM((n_tp, seq, w), BF16),
                pltpu.VMEM((seq, hid), BF16),
                pltpu.VMEM((seq, hid), BF16),
                pltpu.VMEM((seq, width), BF16),
                pltpu.VMEM((dw, hid), BF16),
                pltpu.VMEM((dw, hid), BF16),
                pltpu.VMEM((n_fs, hid, dw), BF16),
                pltpu.VMEM((3, hid, dw), BF16),
                pltpu.VMEM((3, hid, dw), BF16),
                pltpu.VMEM((seq, hid), BF16),
                pltpu.VMEM((seq, hid), BF16),
                pltpu.VMEM((n_tp, seq, w), BF16),
                pltpu.VMEM((n_tp - 1, seq, w), BF16),
                pltpu.VMEM((n_rep, 8, hid), F32),
                dma((n_tp - 1,)),
                dma((n_tp - 1,)),
                dma((nj,)),
                dma((nj,)),
                dma((4,)),
                dma((nj,)),
                dma((n_fs - 1, nj)),
                dma((n_fs - 1, nj)),
                dma((3, 2 * nj)),
                dma((3, 2 * nj)),
                dma((3, 2 * nj)),
                dma((3, 2 * nj)),
                dma((n_tp - 1,)),
                dma((n_tp - 1,)),
                dma((n_rep - 1,)),
                dma((n_rep - 1,)),
            ],
            compiler_params=pltpu.CompilerParams(
                collective_id=0, has_side_effects=True, vmem_limit_bytes=52 * 2**20
            ),
        )(layer_input, gate_saved, up_saved, out_grad, conv_taps, w_gate, w_up, w_down)
        grads, input_grad, taps = (pltpu.with_memory_space_constraint(v, pltpu.VMEM) for v in (grads, input_grad, taps))
        step = 2 * CH if hid % (2 * CH) == 0 else CH

        def whole(shape):
            return pl.BlockSpec(shape, lambda i: (0, 0))
        wide = pl.BlockSpec((dw, step), lambda i: (0, i))
        return pl.pallas_call(
            widen,
            grid=(hid // step,),
            out_shape=(
                jax.ShapeDtypeStruct((seq, w), BF16),
                jax.ShapeDtypeStruct((dw, hid), F32),
                jax.ShapeDtypeStruct((dw, hid), F32),
                jax.ShapeDtypeStruct((hid, dw), F32),
                jax.ShapeDtypeStruct((3, hid), F32),
            ),
            in_specs=[
                pl.BlockSpec((3, step, dw), lambda i: (0, i, 0)), whole((seq, w)), whole((8, hid)),
            ],
            out_specs=(
                whole((seq, w)), wide, wide, pl.BlockSpec((step, dw), lambda i: (i, 0)), whole((3, hid)),
            ),
            compiler_params=pltpu.CompilerParams(vmem_limit_bytes=24 * 2**20),
        )(grads, input_grad, taps)

    return jax.shard_map(
        local,
        mesh=mesh,
        in_specs=(
            P("rep", ("fs", "tp")), P("rep", "tp"), P("rep", "tp"), P("rep", None),
            P(None, "tp"), P("fs", "tp"), P("fs", "tp"), P("tp", "fs"),
        ),
        out_specs=(P("rep", ("fs", "tp")), P("fs", "tp"), P("fs", "tp"), P("tp", "fs"), P(None, "tp")),
        check_vma=False,
    )
```

```python
import functools

import jax
import jax.numpy as jnp
from jax import lax
from jax.experimental import pallas as pl
from jax.experimental.pallas import tpu as pltpu
from jax.sharding import PartitionSpec as P

MESH = pl.DeviceIdType.MESH
F32 = jnp.float32
BF16 = jnp.bfloat16
CH = 128
SUB = 4
HALF = CH // SUB
LAG = 3
WIDE = 128


def kernel(n_rep, n_fs, n_tp, x_in, gate_in, up_in, og_in, taps_in, wg_in, wu_in, wd_in,
           from_in, ig_out, taps_out,
           xb, gate, up, og, wt, wg, wu, wd, act, part, from_out, gp, upp, terms, terms_in, taps_own, taps_all,
           xs_sem, xr_sem, gl_sem, ul_sem, ld_sem, wl_sem, ws_sem, wr_sem,
           in_s, in_r, out_s, out_r, ts_sem, tr_sem, ps_sem, pr_sem):
    rep, fs, tp = lax.axis_index("rep"), lax.axis_index("fs"), lax.axis_index("tp")
    seq, hid = gate.shape
    dw = wd_in.shape[1]
    w = x_in.shape[1]
    nj = hid // CH
    half = n_rep // 2
    low = rep < half
    depth = jnp.where(low, rep, n_rep - 1 - rep)
    inward = jnp.where(low, rep + 1, rep - 1)
    outward = jnp.where(low, rep - 1, rep + 1)
    has_out = depth > 0
    outward = jnp.where(has_out, outward, inward)
    innermost = depth == half - 1
    lag = LAG + 9 * SUB * (half - 1 - depth)
    lead = min(4, nj)
    steps = 3 * nj
    rest_end = lead - 1 + 2 * (nj - lead) + lead
    turns = max(steps + -(-LAG // SUB) + 9 * (half - 1), rest_end + n_tp + 5)

    def rows(j):
        return pl.ds(pl.multiple_of(j * CH, CH), CH)

    def piece(i):
        return pl.ds(pl.multiple_of(i * HALF, HALF), HALF)

    def unit(i):
        v, h = lax.div(i, SUB), lax.rem(i, SUB)
        a = v - lead
        b = a - 3 * (nj - lead)
        m = lax.rem(a, 3)
        mid = a < 3 * (nj - lead)
        first = a < 0
        k = jnp.where(first, 0, jnp.where(mid, jnp.where(m == 2, 0, m + 1), 1 + lax.rem(b, 2)))
        j = jnp.where(first, v, jnp.where(
            mid, lax.div(a, 3) + jnp.where(m == 2, lead, 0), nj - lead + lax.div(b, 2)))
        return SUB * j + h, k

    def fs_peer(d):
        return lax.rem(fs + d, n_fs)

    def tp_peer(d):
        return lax.rem(tp + d, n_tp)

    def load_gate(j):
        return pltpu.make_async_copy(gate_in.at[:, rows(j)], gate.at[:, rows(j)], gl_sem.at[j])

    def load_up(j):
        return pltpu.make_async_copy(up_in.at[:, rows(j)], up.at[:, rows(j)], ul_sem.at[j])

    def load_wd(j):
        return pltpu.make_async_copy(wd_in.at[rows(j), :], wd.at[fs, rows(j), :], wl_sem.at[j])

    def send_wd(j, d):
        return pltpu.make_async_remote_copy(
            src_ref=wd_in.at[rows(j), :], dst_ref=wd.at[fs, rows(j), :],
            send_sem=ws_sem.at[d - 1], recv_sem=wr_sem.at[d - 1, j],
            device_id={"fs": fs_peer(d)}, device_id_type=MESH)

    def recv_wd(j, d):
        src = lax.rem(fs + n_fs - d, n_fs)
        return pltpu.make_async_remote_copy(
            src_ref=wd_in.at[rows(j), :], dst_ref=wd.at[src, rows(j), :],
            send_sem=ws_sem.at[d - 1], recv_sem=wr_sem.at[d - 1, j],
            device_id={"fs": fs_peer(d)}, device_id_type=MESH)

    def x_copy(d, slot):
        return pltpu.make_async_remote_copy(
            src_ref=x_in, dst_ref=xb.at[slot], send_sem=xs_sem.at[d - 1], recv_sem=xr_sem.at[d - 1],
            device_id={"tp": tp_peer(d)}, device_id_type=MESH)

    def term_copy(d):
        return pltpu.make_async_remote_copy(
            src_ref=terms.at[tp_peer(d)], dst_ref=terms_in.at[d - 1],
            send_sem=ts_sem.at[d - 1], recv_sem=tr_sem.at[d - 1],
            device_id={"tp": tp_peer(d)}, device_id_type=MESH)

    def taps_copy(d, slot):
        return pltpu.make_async_remote_copy(
            src_ref=taps_all.at[rep], dst_ref=taps_all.at[slot],
            send_sem=ps_sem.at[d - 1], recv_sem=pr_sem.at[d - 1],
            device_id={"rep": lax.rem(rep + d, n_rep)}, device_id_type=MESH)

    def in_copy(j, k, dst):
        return pltpu.make_async_remote_copy(
            src_ref=part.at[k, piece(j), :], dst_ref=dst.at[k, piece(j), :],
            send_sem=in_s.at[k], recv_sem=(in_r if dst is from_out else out_r).at[k, j],
            device_id={"rep": inward}, device_id_type=MESH)

    def out_copy(j, k):
        return pltpu.make_async_remote_copy(
            src_ref=from_in.at[k, piece(j), :], dst_ref=from_in.at[k, piece(j), :],
            send_sem=out_s.at[k], recv_sem=out_r.at[k, j],
            device_id={"rep": outward}, device_id_type=MESH)

    def og_copy(d):
        cols = pl.ds(pl.multiple_of(fs_peer(d) * dw, dw), dw)
        return pltpu.make_async_copy(og_in.at[:, cols], og.at[:, cols], ld_sem.at[4 + d])

    loads = [
        pltpu.make_async_copy(taps_in, wt, ld_sem.at[0]),
        pltpu.make_async_copy(wg_in, wg, ld_sem.at[1]),
        pltpu.make_async_copy(wu_in, wu, ld_sem.at[2]),
        pltpu.make_async_copy(x_in, xb.at[tp], ld_sem.at[3]),
    ]
    taps_own[...] = jnp.zeros_like(taps_own)
    load_gate(0).start()
    load_up(0).start()
    loads[0].start()
    og_copy(0).start()

    barrier = pltpu.get_barrier_semaphore()
    for axis, n, me in (("rep", n_rep, rep), ("fs", n_fs, fs), ("tp", n_tp, tp)):
        for d in range(1, n):
            pl.semaphore_signal(barrier, inc=1, device_id={axis: lax.rem(me + d, n)}, device_id_type=MESH)
    for d in range(1, n_fs):
        og_copy(d).start()

    pos = lax.broadcasted_iota(jnp.int32, (seq, CH), 0)

    def back(v, n):
        return jnp.where(pos >= n, pltpu.roll(v, n, 0), 0.0)

    def ahead(v, n):
        return jnp.where(pos < seq - n, pltpu.roll(v, seq - n, 0), 0.0)

    def conv(j):
        g = gate[:, rows(j)].astype(F32)
        t = wt[:, rows(j)].astype(F32)
        b1, b2 = back(g, 1), back(g, 2)
        return g, b1, b2, t, t[0:1] * b2 + t[1:2] * b1 + t[2:3] * g

    tdot = functools.partial(lax.dot_general, dimension_numbers=(((0,), (0,)), ((), ())),
                             preferred_element_type=F32)
    wdot = functools.partial(lax.dot_general, dimension_numbers=(((1,), (1,)), ((), ())),
                             preferred_element_type=F32)

    own = pl.ds(pl.multiple_of(fs * dw, dw), dw)

    def down_first(j):
        load_gate(j).wait()
        load_up(j).wait()
        co = conv(j)[4]
        act[...] = (co * jax.nn.sigmoid(co) * up[:, rows(j)].astype(F32)).astype(BF16)

    def down_second(j):
        part[0, rows(j), :] = tdot(act[...], og[:, own]).astype(BF16)

    def rest_first(j):
        load_wd(j).wait()
        for d in range(1, n_fs):
            recv_wd(j, d).wait_recv()
        ag = wdot(og[:, 0:dw], wd[0, rows(j), :])
        for f in range(1, n_fs):
            ag = ag + wdot(og[:, f * dw:(f + 1) * dw], wd[f, rows(j), :])
        g, b1, b2, t, co = conv(j)
        s = jax.nn.sigmoid(co)
        upp[:, rows(j)] = (ag * (co * s)).astype(BF16)
        cg = ag * up[:, rows(j)].astype(F32) * s * (1.0 + co * (1.0 - s))
        gp[:, rows(j)] = (t[0:1] * ahead(cg, 2) + t[1:2] * ahead(cg, 1) + t[2:3] * cg).astype(BF16)
        for k, v in enumerate((b2, b1, g)):
            taps_own[pl.ds(3 * j + k, 1), :] = jnp.sum(cg * v, axis=0, keepdims=True)

    def rest_second(j):
        @pl.when(j == 0)
        def _():
            loads[3].wait()
            for d in range(1, n_tp):
                x_copy(d, lax.rem(tp + n_tp - d, n_tp)).wait_recv()
        g_part, u_part = gp[:, rows(j)], upp[:, rows(j)]
        for b in range(n_tp):
            part[1, rows(j), b * w:(b + 1) * w] = tdot(g_part, xb[b]).astype(BF16)
            part[2, rows(j), b * w:(b + 1) * w] = tdot(u_part, xb[b]).astype(BF16)

    def term_half(d, h):
        if h == 0:
            @pl.when(d == 1)
            def _():
                taps_all[rep] = taps_own[...].astype(BF16)
                for p in range(1, n_rep):
                    taps_copy(p, rep).start()
                loads[1].wait()
                loads[2].wait()
        b = tp_peer(d)
        r = pl.ds(pl.multiple_of(b * w, w), w)
        t = pl.ds(h * (seq // 2), seq // 2)
        terms[b, t, :] = (wdot(gp[t, :], wg[r, :]) + wdot(upp[t, :], wu[r, :])).astype(BF16)
        if h == 1:
            @pl.when(d < n_tp)
            def _():
                term_copy(d).start()

    def finish():
        total = terms[tp].astype(F32)
        for d in range(1, n_tp):
            term_copy(d).wait_recv()
            total = total + terms_in[d - 1].astype(F32)
        ig_out[...] = total.astype(BF16)
        for d in range(1, n_rep):
            taps_copy(d, lax.rem(rep + n_rep - d, n_rep)).wait_recv()
        acc = taps_all[0].astype(F32)
        for i in range(1, n_rep):
            acc = acc + taps_all[i].astype(F32)
        taps_own[...] = acc
        for j in range(nj):
            taps_out[0:3, j * CH:(j + 1) * CH] = taps_own[3 * j:3 * j + 3, :]
        for d in range(1, n_tp):
            x_copy(d, tp).wait_send()
            term_copy(d).wait_send()
        for d in range(1, n_rep):
            taps_copy(d, rep).wait_send()
        for d in range(1, n_fs):
            pltpu.make_async_remote_copy(
                src_ref=wd_in, dst_ref=wd.at[fs], send_sem=ws_sem.at[d - 1], recv_sem=wr_sem.at[d - 1, 0],
                device_id={"fs": fs_peer(d)}, device_id_type=MESH).wait_send()

    def q_stage(j, k):
        @pl.when(has_out)
        def _():
            in_copy(j, k, from_out).wait_recv()
            r = piece(j)
            part[k, r, :] = (part[k, r, :].astype(F32) + from_out[k, r, :].astype(F32)).astype(BF16)

        @pl.when(innermost)
        def _():
            in_copy(j, k, from_in).start()

        @pl.when(jnp.logical_not(innermost))
        def _():
            in_copy(j, k, from_out).start()

    def s_stage(j, k):
        out_copy(j, k).wait_recv()

        @pl.when(innermost)
        def _():
            r = piece(j)
            from_in[k, r, :] = (part[k, r, :].astype(F32) + from_in[k, r, :].astype(F32)).astype(BF16)

        @pl.when(has_out)
        def _():
            out_copy(j, k).start()

    def load_rest(j, c):
        load_gate(j).start()
        load_up(j).start()
        return c
    lax.fori_loop(1, nj, load_rest, 0)
    loads[0].wait()
    down_first(0)
    og_copy(0).wait()
    down_second(0)
    pl.semaphore_wait(barrier, n_rep + n_fs + n_tp - 3)

    @pl.when(jnp.logical_not(has_out))
    def _():
        for h in range(SUB):
            q_stage(h, 0)
    for d in range(1, n_tp):
        x_copy(d, tp).start()

    def weights(j, c):
        for d in range(1, n_fs):
            send_wd(j, d).start()
        load_wd(j).start()
        return c
    lax.fori_loop(0, nj, weights, 0)
    for load in loads[1:]:
        load.start()
    for d in range(1, n_fs):
        og_copy(d).wait()

    def step(v, c):
        a = v - (lead - 1)
        b = a - 2 * (nj - lead)
        early = a < 0
        mid = jnp.logical_and(a >= 0, b < 0)
        is_down = jnp.logical_or(early, jnp.logical_and(mid, lax.rem(a, 2) == 1))
        is_rest = jnp.logical_and(jnp.logical_not(is_down), b < lead)
        is_term = jnp.logical_and(b >= lead, b < lead + n_tp)
        down_j = jnp.where(early, v + 1, lead + lax.div(a, 2))
        rest_j = jnp.where(mid, lax.div(a, 2), nj - lead + b)
        for h in range(SUB):
            i = SUB * v + h

            @pl.when(jnp.logical_and(v < steps, jnp.logical_or(v > 0, has_out)))
            def _():
                q_stage(*unit(i))
            si = i - lag

            @pl.when(jnp.logical_and(si >= 0, si < SUB * steps))
            def _():
                s_stage(*unit(si))

            turn = {0: 0, SUB // 2: 1}.get(h)
            if turn is None:
                continue

            @pl.when(is_down)
            def _():
                (down_first, down_second)[turn](down_j)

            @pl.when(is_rest)
            def _():
                (rest_first, rest_second)[turn](rest_j)

            @pl.when(is_term)
            def _():
                term_half(b - lead + 1, turn)

        @pl.when(v == rest_end + n_tp + 4)
        def _():
            finish()
        return c
    lax.fori_loop(0, turns, step, 0)

    for k in range(3):
        pltpu.make_async_remote_copy(
            src_ref=part.at[k], dst_ref=from_out.at[k], send_sem=in_s.at[k], recv_sem=in_r.at[k, 0],
            device_id={"rep": inward}, device_id_type=MESH).wait_send()

        @pl.when(has_out)
        def _():
            pltpu.make_async_remote_copy(
                src_ref=from_in.at[k], dst_ref=from_in.at[k], send_sem=out_s.at[k], recv_sem=out_r.at[k, 0],
                device_id={"rep": outward}, device_id_type=MESH).wait_send()


def widen(grads, input_grad, taps, ig_out, gate_out, up_out, down_out, taps_out, ring, ring_t, d_sem, t_sem, s_sem):
    hid, dw = down_out.shape
    slots = ring.shape[0]
    small = [
        pltpu.make_async_copy(input_grad, ig_out, s_sem.at[0]),
        pltpu.make_async_copy(taps.at[0:3, :], taps_out, s_sem.at[1]),
    ]
    for copy in small:
        copy.start()

    def down(i, s):
        return pltpu.make_async_copy(ring.at[s], down_out.at[pl.ds(i * WIDE, WIDE), :], d_sem.at[s])

    def wide(out, i, s):
        return pltpu.make_async_copy(ring_t.at[s], out.at[:, pl.ds(i * WIDE, WIDE)], t_sem.at[s])

    n = hid // WIDE
    for i in range(n):
        r = slice(i * WIDE, (i + 1) * WIDE)
        s = i % slots
        if i >= slots:
            down(i - slots, s).wait()
            wide(gate_out, i - slots, 2 * s).wait()
            wide(up_out, i - slots, 2 * s + 1).wait()
        ring[s] = grads[0, r, :].astype(F32)
        down(i, s).start()
        ring_t[2 * s] = grads[1, r, :].astype(F32).T
        wide(gate_out, i, 2 * s).start()
        ring_t[2 * s + 1] = grads[2, r, :].astype(F32).T
        wide(up_out, i, 2 * s + 1).start()
    for i in range(max(n - slots, 0), n):
        s = i % slots
        down(i, s).wait()
        wide(gate_out, i, 2 * s).wait()
        wide(up_out, i, 2 * s + 1).wait()
    for copy in small:
        copy.wait()


def solution(mesh):
    n_rep, n_fs, n_tp = mesh.shape["rep"], mesh.shape["fs"], mesh.shape["tp"]

    def local(layer_input, gate_saved, up_saved, out_grad, conv_taps, w_gate, w_up, w_down):
        seq, w = layer_input.shape
        dw, hid = w_gate.shape
        width = out_grad.shape[1]
        nj = hid // CH
        tap_rows = -(-3 * nj // 16) * 16
        any_spec = pl.BlockSpec(memory_space=pl.ANY)
        vmem = pl.BlockSpec(memory_space=pltpu.VMEM)
        dma = pltpu.SemaphoreType.DMA
        grads, input_grad, taps = pl.pallas_call(
            functools.partial(kernel, n_rep, n_fs, n_tp),
            out_shape=(
                pltpu.VMEM((3, hid, dw), BF16),
                pltpu.VMEM((seq, w), BF16),
                pltpu.VMEM((8, hid), F32),
            ),
            in_specs=[any_spec] * 8,
            out_specs=(vmem, vmem, vmem),
            scratch_shapes=[
                pltpu.VMEM((n_tp, seq, w), BF16),
                pltpu.VMEM((seq, hid), BF16),
                pltpu.VMEM((seq, hid), BF16),
                pltpu.VMEM((seq, width), BF16),
                pltpu.VMEM((3, hid), BF16),
                pltpu.VMEM((dw, hid), BF16),
                pltpu.VMEM((dw, hid), BF16),
                pltpu.VMEM((n_fs, hid, dw), BF16),
                pltpu.VMEM((seq, CH), BF16),
                pltpu.VMEM((3, hid, dw), BF16),
                pltpu.VMEM((3, hid, dw), BF16),
                pltpu.VMEM((seq, hid), BF16),
                pltpu.VMEM((seq, hid), BF16),
                pltpu.VMEM((n_tp, seq, w), BF16),
                pltpu.VMEM((n_tp - 1, seq, w), BF16),
                pltpu.VMEM((tap_rows, CH), F32),
                pltpu.VMEM((n_rep, tap_rows, CH), BF16),
                dma((n_tp - 1,)),
                dma((n_tp - 1,)),
                dma((nj,)),
                dma((nj,)),
                dma((4 + n_fs,)),
                dma((nj,)),
                dma((n_fs - 1,)),
                dma((n_fs - 1, nj)),
                dma((3,)),
                dma((3, SUB * nj)),
                dma((3,)),
                dma((3, SUB * nj)),
                dma((n_tp - 1,)),
                dma((n_tp - 1,)),
                dma((n_rep - 1,)),
                dma((n_rep - 1,)),
            ],
            compiler_params=pltpu.CompilerParams(
                collective_id=0, has_side_effects=True, vmem_limit_bytes=52 * 2**20
            ),
        )(layer_input, gate_saved, up_saved, out_grad, conv_taps, w_gate, w_up, w_down)
        grads, input_grad, taps = (pltpu.with_memory_space_constraint(v, pltpu.VMEM) for v in (grads, input_grad, taps))
        slots = min(4, hid // WIDE)
        return pl.pallas_call(
            widen,
            out_shape=(
                jax.ShapeDtypeStruct((seq, w), BF16),
                jax.ShapeDtypeStruct((dw, hid), F32),
                jax.ShapeDtypeStruct((dw, hid), F32),
                jax.ShapeDtypeStruct((hid, dw), F32),
                jax.ShapeDtypeStruct((3, hid), F32),
            ),
            in_specs=[vmem] * 3,
            out_specs=[any_spec] * 5,
            scratch_shapes=[
                pltpu.VMEM((slots, WIDE, dw), F32),
                pltpu.VMEM((2 * slots, dw, WIDE), F32),
                dma((slots,)),
                dma((2 * slots,)),
                dma((2,)),
            ],
            compiler_params=pltpu.CompilerParams(vmem_limit_bytes=24 * 2**20),
        )(grads, input_grad, taps)

    return jax.shard_map(
        local,
        mesh=mesh,
        in_specs=(
            P("rep", ("fs", "tp")), P("rep", "tp"), P("rep", "tp"), P("rep", None),
            P(None, "tp"), P("fs", "tp"), P("fs", "tp"), P("tp", "fs"),
        ),
        out_specs=(P("rep", ("fs", "tp")), P("fs", "tp"), P("fs", "tp"), P("tp", "fs"), P(None, "tp")),
        check_vma=False,
    )
```

```python
import functools

import jax
import jax.numpy as jnp
from jax import lax
from jax.experimental import pallas as pl
from jax.experimental.pallas import tpu as pltpu
from jax.sharding import PartitionSpec as P

MESH = pl.DeviceIdType.MESH
F32 = jnp.float32
BF16 = jnp.bfloat16
CH = 128
SUB = 4
HALF = CH // SUB
LAG = 2
HOP = 3
WIDE = 128


def kernel(n_rep, n_fs, n_tp, x_in, gate_in, up_in, og_in, taps_in, wg_in, wu_in, wd_in,
           from_in, ig_out, taps_out,
           xb, gate, up, og, wt, wg, wu, wd, act, part, from_out, gp, upp, terms, terms_in, taps_own, taps_all,
           xs_sem, xr_sem, gl_sem, ul_sem, ld_sem, wl_sem, ws_sem, wr_sem,
           in_s, in_r, out_s, out_r, ts_sem, tr_sem, ps_sem, pr_sem):
    rep, fs, tp = lax.axis_index("rep"), lax.axis_index("fs"), lax.axis_index("tp")
    seq, hid = gate.shape
    dw = wd_in.shape[1]
    w = x_in.shape[1]
    nj = hid // CH
    half = n_rep // 2
    low = rep < half
    depth = jnp.where(low, rep, n_rep - 1 - rep)
    inward = jnp.where(low, rep + 1, rep - 1)
    outward = jnp.where(low, rep - 1, rep + 1)
    has_out = depth > 0
    outward = jnp.where(has_out, outward, inward)
    innermost = depth == half - 1
    lag = LAG + HOP * SUB * (half - 1 - depth)
    lead = min(4, nj)
    steps = 3 * nj
    ring = in_r.shape[0]
    rest_end = lead - 1 + 2 * (nj - lead) + lead
    turns = max(steps + -(-LAG // SUB) + HOP * (half - 1), rest_end + n_tp + 5)

    def rows(j):
        return pl.ds(pl.multiple_of(j * CH, CH), CH)

    def piece(i):
        return pl.ds(pl.multiple_of(i * HALF, HALF), HALF)

    def unit(i):
        v, h = lax.div(i, SUB), lax.rem(i, SUB)
        a = v - lead
        b = a - 3 * (nj - lead)
        m = lax.rem(a, 3)
        mid = a < 3 * (nj - lead)
        first = a < 0
        k = jnp.where(first, 0, jnp.where(mid, jnp.where(m == 2, 0, m + 1), 1 + lax.rem(b, 2)))
        j = jnp.where(first, v, jnp.where(
            mid, lax.div(a, 3) + jnp.where(m == 2, lead, 0), nj - lead + lax.div(b, 2)))
        return SUB * j + h, k

    def fs_peer(d):
        return lax.rem(fs + d, n_fs)

    def tp_peer(d):
        return lax.rem(tp + d, n_tp)

    def load_gate(p):
        c = slice(0, CH) if p == 0 else slice(CH, hid)
        return pltpu.make_async_copy(gate_in.at[:, c], gate.at[:, c], gl_sem.at[p])

    def load_up(p):
        c = slice(0, CH) if p == 0 else slice(CH, hid)
        return pltpu.make_async_copy(up_in.at[:, c], up.at[:, c], ul_sem.at[p])

    load_wd = pltpu.make_async_copy(wd_in, wd.at[fs], wl_sem.at[0])

    def send_wd(j, d):
        return pltpu.make_async_remote_copy(
            src_ref=wd_in.at[rows(j), :], dst_ref=wd.at[fs, rows(j), :],
            send_sem=ws_sem.at[d - 1], recv_sem=wr_sem.at[d - 1, j],
            device_id={"fs": fs_peer(d)}, device_id_type=MESH)

    def recv_wd(j, d):
        src = lax.rem(fs + n_fs - d, n_fs)
        return pltpu.make_async_remote_copy(
            src_ref=wd_in.at[rows(j), :], dst_ref=wd.at[src, rows(j), :],
            send_sem=ws_sem.at[d - 1], recv_sem=wr_sem.at[d - 1, j],
            device_id={"fs": fs_peer(d)}, device_id_type=MESH)

    def x_copy(d, slot):
        return pltpu.make_async_remote_copy(
            src_ref=x_in, dst_ref=xb.at[slot], send_sem=xs_sem.at[d - 1], recv_sem=xr_sem.at[d - 1],
            device_id={"tp": tp_peer(d)}, device_id_type=MESH)

    def term_copy(d):
        return pltpu.make_async_remote_copy(
            src_ref=terms.at[tp_peer(d)], dst_ref=terms_in.at[d - 1],
            send_sem=ts_sem.at[d - 1], recv_sem=tr_sem.at[d - 1],
            device_id={"tp": tp_peer(d)}, device_id_type=MESH)

    def taps_copy(d, slot):
        return pltpu.make_async_remote_copy(
            src_ref=taps_all.at[rep], dst_ref=taps_all.at[slot],
            send_sem=ps_sem.at[d - 1], recv_sem=pr_sem.at[d - 1],
            device_id={"rep": lax.rem(rep + d, n_rep)}, device_id_type=MESH)

    def in_copy(i, j, k, dst):
        return pltpu.make_async_remote_copy(
            src_ref=part.at[k, piece(j), :], dst_ref=dst.at[k, piece(j), :],
            send_sem=in_s.at[k], recv_sem=(in_r if dst is from_out else out_r).at[lax.rem(i, ring)],
            device_id={"rep": inward}, device_id_type=MESH)

    def out_copy(i, j, k):
        return pltpu.make_async_remote_copy(
            src_ref=from_in.at[k, piece(j), :], dst_ref=from_in.at[k, piece(j), :],
            send_sem=out_s.at[k], recv_sem=out_r.at[lax.rem(i, ring)],
            device_id={"rep": outward}, device_id_type=MESH)

    def og_copy(d):
        cols = pl.ds(pl.multiple_of(fs_peer(d) * dw, dw), dw)
        return pltpu.make_async_copy(og_in.at[:, cols], og.at[:, cols], ld_sem.at[4 + d])

    loads = [
        pltpu.make_async_copy(taps_in, wt, ld_sem.at[0]),
        pltpu.make_async_copy(wg_in, wg, ld_sem.at[1]),
        pltpu.make_async_copy(wu_in, wu, ld_sem.at[2]),
        pltpu.make_async_copy(x_in, xb.at[tp], ld_sem.at[3]),
    ]
    taps_own[...] = jnp.zeros_like(taps_own)
    load_gate(0).start()
    load_up(0).start()
    loads[0].start()
    og_copy(0).start()

    barrier = pltpu.get_barrier_semaphore()
    for axis, n, me in (("rep", n_rep, rep), ("fs", n_fs, fs), ("tp", n_tp, tp)):
        for d in range(1, n):
            pl.semaphore_signal(barrier, inc=1, device_id={axis: lax.rem(me + d, n)}, device_id_type=MESH)
    for d in range(1, n_fs):
        og_copy(d).start()

    pos = lax.broadcasted_iota(jnp.int32, (seq, CH), 0)

    def back(v, n):
        return jnp.where(pos >= n, pltpu.roll(v, n, 0), 0.0)

    def ahead(v, n):
        return jnp.where(pos < seq - n, pltpu.roll(v, seq - n, 0), 0.0)

    def conv(j):
        g = gate[:, rows(j)].astype(F32)
        t = wt[:, rows(j)].astype(F32)
        b1, b2 = back(g, 1), back(g, 2)
        return g, b1, b2, t, t[0:1] * b2 + t[1:2] * b1 + t[2:3] * g

    tdot = functools.partial(lax.dot_general, dimension_numbers=(((0,), (0,)), ((), ())),
                             preferred_element_type=F32)
    wdot = functools.partial(lax.dot_general, dimension_numbers=(((1,), (1,)), ((), ())),
                             preferred_element_type=F32)

    own = pl.ds(pl.multiple_of(fs * dw, dw), dw)

    def down_first(j):
        @pl.when(j == 1)
        def _():
            load_gate(1).wait()
            load_up(1).wait()
        co = conv(j)[4]
        act[...] = (co * jax.nn.sigmoid(co) * up[:, rows(j)].astype(F32)).astype(BF16)

    def down_second(j):
        part[0, rows(j), :] = tdot(act[...], og[:, own]).astype(BF16)

    def rest_first(j):
        @pl.when(j == 0)
        def _():
            load_wd.wait()
        for d in range(1, n_fs):
            recv_wd(j, d).wait_recv()
        ag = wdot(og[:, 0:dw], wd[0, rows(j), :])
        for f in range(1, n_fs):
            ag = ag + wdot(og[:, f * dw:(f + 1) * dw], wd[f, rows(j), :])
        g, b1, b2, t, co = conv(j)
        s = jax.nn.sigmoid(co)
        upp[:, rows(j)] = (ag * (co * s)).astype(BF16)
        cg = ag * up[:, rows(j)].astype(F32) * s * (1.0 + co * (1.0 - s))
        gp[:, rows(j)] = (t[0:1] * ahead(cg, 2) + t[1:2] * ahead(cg, 1) + t[2:3] * cg).astype(BF16)
        for k, v in enumerate((b2, b1, g)):
            taps_own[pl.ds(3 * j + k, 1), :] = jnp.sum(cg * v, axis=0, keepdims=True)

    def rest_second(j):
        @pl.when(j == 0)
        def _():
            loads[3].wait()
            for d in range(1, n_tp):
                x_copy(d, lax.rem(tp + n_tp - d, n_tp)).wait_recv()
        g_part, u_part = gp[:, rows(j)], upp[:, rows(j)]
        for b in range(n_tp):
            part[1, rows(j), b * w:(b + 1) * w] = tdot(g_part, xb[b]).astype(BF16)
            part[2, rows(j), b * w:(b + 1) * w] = tdot(u_part, xb[b]).astype(BF16)

    def term_half(d, h):
        if h == 0:
            @pl.when(d == 1)
            def _():
                taps_all[rep] = taps_own[...].astype(BF16)
                for p in range(1, n_rep):
                    taps_copy(p, rep).start()
                loads[1].wait()
                loads[2].wait()
        b = tp_peer(d)
        r = pl.ds(pl.multiple_of(b * w, w), w)
        t = pl.ds(h * (seq // 2), seq // 2)
        terms[b, t, :] = (wdot(gp[t, :], wg[r, :]) + wdot(upp[t, :], wu[r, :])).astype(BF16)
        if h == 1:
            @pl.when(d < n_tp)
            def _():
                term_copy(d).start()

    def finish():
        total = terms[tp].astype(F32)
        for d in range(1, n_tp):
            term_copy(d).wait_recv()
            total = total + terms_in[d - 1].astype(F32)
        ig_out[...] = total.astype(BF16)
        for d in range(1, n_rep):
            taps_copy(d, lax.rem(rep + n_rep - d, n_rep)).wait_recv()
        acc = taps_all[0].astype(F32)
        for i in range(1, n_rep):
            acc = acc + taps_all[i].astype(F32)
        taps_own[...] = acc
        for j in range(nj):
            taps_out[0:3, j * CH:(j + 1) * CH] = taps_own[3 * j:3 * j + 3, :]
        for d in range(1, n_tp):
            x_copy(d, tp).wait_send()
            term_copy(d).wait_send()
        for d in range(1, n_rep):
            taps_copy(d, rep).wait_send()
        for d in range(1, n_fs):
            pltpu.make_async_remote_copy(
                src_ref=wd_in, dst_ref=wd.at[fs], send_sem=ws_sem.at[d - 1], recv_sem=wr_sem.at[d - 1, 0],
                device_id={"fs": fs_peer(d)}, device_id_type=MESH).wait_send()

    def q_stage(i):
        j, k = unit(i)

        @pl.when(has_out)
        def _():
            in_copy(i, j, k, from_out).wait_recv()
            r = piece(j)
            part[k, r, :] = (part[k, r, :].astype(F32) + from_out[k, r, :].astype(F32)).astype(BF16)

        @pl.when(innermost)
        def _():
            in_copy(i, j, k, from_in).start()

        @pl.when(jnp.logical_not(innermost))
        def _():
            in_copy(i, j, k, from_out).start()

    def s_stage(i):
        j, k = unit(i)
        out_copy(i, j, k).wait_recv()

        @pl.when(innermost)
        def _():
            r = piece(j)
            from_in[k, r, :] = (part[k, r, :].astype(F32) + from_in[k, r, :].astype(F32)).astype(BF16)

        @pl.when(has_out)
        def _():
            out_copy(i, j, k).start()

    load_gate(1).start()
    load_up(1).start()
    loads[0].wait()
    load_gate(0).wait()
    load_up(0).wait()
    down_first(0)
    og_copy(0).wait()
    down_second(0)
    pl.semaphore_wait(barrier, n_rep + n_fs + n_tp - 3)

    @pl.when(jnp.logical_not(has_out))
    def _():
        for h in range(SUB):
            q_stage(jnp.int32(h))
    for d in range(1, n_tp):
        x_copy(d, tp).start()

    def weights(j, c):
        for d in range(1, n_fs):
            send_wd(j, d).start()
        return c
    load_wd.start()
    lax.fori_loop(0, nj, weights, 0)
    for load in loads[1:]:
        load.start()
    for d in range(1, n_fs):
        og_copy(d).wait()

    def step(v, c):
        a = v - (lead - 1)
        b = a - 2 * (nj - lead)
        early = a < 0
        mid = jnp.logical_and(a >= 0, b < 0)
        is_down = jnp.logical_or(early, jnp.logical_and(mid, lax.rem(a, 2) == 1))
        is_rest = jnp.logical_and(jnp.logical_not(is_down), b < lead)
        is_term = jnp.logical_and(b >= lead, b < lead + n_tp)
        down_j = jnp.where(early, v + 1, lead + lax.div(a, 2))
        rest_j = jnp.where(mid, lax.div(a, 2), nj - lead + b)
        for h in range(SUB):
            i = SUB * v + h

            @pl.when(jnp.logical_and(v < steps, jnp.logical_or(v > 0, has_out)))
            def _():
                q_stage(i)
            turn = {0: 0, SUB // 2: 1}.get(h)
            if turn is not None:
                @pl.when(is_down)
                def _():
                    (down_first, down_second)[turn](down_j)

                @pl.when(is_rest)
                def _():
                    (rest_first, rest_second)[turn](rest_j)

                @pl.when(is_term)
                def _():
                    term_half(b - lead + 1, turn)

            si = i - lag

            @pl.when(jnp.logical_and(si >= 0, si < SUB * steps))
            def _():
                s_stage(si)

        @pl.when(v == rest_end + n_tp + 4)
        def _():
            finish()
        return c
    lax.fori_loop(0, turns, step, 0)

    for k in range(3):
        pltpu.make_async_remote_copy(
            src_ref=part.at[k], dst_ref=from_out.at[k], send_sem=in_s.at[k], recv_sem=in_r.at[0],
            device_id={"rep": inward}, device_id_type=MESH).wait_send()

        @pl.when(has_out)
        def _():
            pltpu.make_async_remote_copy(
                src_ref=from_in.at[k], dst_ref=from_in.at[k], send_sem=out_s.at[k], recv_sem=out_r.at[0],
                device_id={"rep": outward}, device_id_type=MESH).wait_send()


def widen(grads, input_grad, taps, ig_out, gate_out, up_out, down_out, taps_out, ring, ring_t, d_sem, t_sem, s_sem):
    hid, dw = down_out.shape
    slots = ring.shape[0]
    small = [
        pltpu.make_async_copy(input_grad, ig_out, s_sem.at[0]),
        pltpu.make_async_copy(taps.at[0:3, :], taps_out, s_sem.at[1]),
    ]
    for copy in small:
        copy.start()

    def down(i, s):
        return pltpu.make_async_copy(ring.at[s], down_out.at[pl.ds(i * WIDE, WIDE), :], d_sem.at[s])

    def wide(out, i, s):
        return pltpu.make_async_copy(ring_t.at[s], out.at[:, pl.ds(i * WIDE, WIDE)], t_sem.at[s])

    n = hid // WIDE
    for i in range(n):
        r = slice(i * WIDE, (i + 1) * WIDE)
        s = i % slots
        if i >= slots:
            down(i - slots, s).wait()
            wide(gate_out, i - slots, 2 * s).wait()
            wide(up_out, i - slots, 2 * s + 1).wait()
        ring[s] = grads[0, r, :].astype(F32)
        down(i, s).start()
        ring_t[2 * s] = grads[1, r, :].astype(F32).T
        wide(gate_out, i, 2 * s).start()
        ring_t[2 * s + 1] = grads[2, r, :].astype(F32).T
        wide(up_out, i, 2 * s + 1).start()
    for i in range(max(n - slots, 0), n):
        s = i % slots
        down(i, s).wait()
        wide(gate_out, i, 2 * s).wait()
        wide(up_out, i, 2 * s + 1).wait()
    for copy in small:
        copy.wait()


def solution(mesh):
    n_rep, n_fs, n_tp = mesh.shape["rep"], mesh.shape["fs"], mesh.shape["tp"]

    def local(layer_input, gate_saved, up_saved, out_grad, conv_taps, w_gate, w_up, w_down):
        seq, w = layer_input.shape
        dw, hid = w_gate.shape
        width = out_grad.shape[1]
        nj = hid // CH
        ring = min(LAG + HOP * SUB * (n_rep // 2 - 1) + 2, 3 * SUB * nj)
        tap_rows = -(-3 * nj // 16) * 16
        any_spec = pl.BlockSpec(memory_space=pl.ANY)
        vmem = pl.BlockSpec(memory_space=pltpu.VMEM)
        dma = pltpu.SemaphoreType.DMA
        grads, input_grad, taps = pl.pallas_call(
            functools.partial(kernel, n_rep, n_fs, n_tp),
            out_shape=(
                pltpu.VMEM((3, hid, dw), BF16),
                pltpu.VMEM((seq, w), BF16),
                pltpu.VMEM((8, hid), F32),
            ),
            in_specs=[any_spec] * 8,
            out_specs=(vmem, vmem, vmem),
            scratch_shapes=[
                pltpu.VMEM((n_tp, seq, w), BF16),
                pltpu.VMEM((seq, hid), BF16),
                pltpu.VMEM((seq, hid), BF16),
                pltpu.VMEM((seq, width), BF16),
                pltpu.VMEM((3, hid), BF16),
                pltpu.VMEM((dw, hid), BF16),
                pltpu.VMEM((dw, hid), BF16),
                pltpu.VMEM((n_fs, hid, dw), BF16),
                pltpu.VMEM((seq, CH), BF16),
                pltpu.VMEM((3, hid, dw), BF16),
                pltpu.VMEM((3, hid, dw), BF16),
                pltpu.VMEM((seq, hid), BF16),
                pltpu.VMEM((seq, hid), BF16),
                pltpu.VMEM((n_tp, seq, w), BF16),
                pltpu.VMEM((n_tp - 1, seq, w), BF16),
                pltpu.VMEM((tap_rows, CH), F32),
                pltpu.VMEM((n_rep, tap_rows, CH), BF16),
                dma((n_tp - 1,)),
                dma((n_tp - 1,)),
                dma((2,)),
                dma((2,)),
                dma((4 + n_fs,)),
                dma((1,)),
                dma((n_fs - 1,)),
                dma((n_fs - 1, nj)),
                dma((3,)),
                dma((ring,)),
                dma((3,)),
                dma((ring,)),
                dma((n_tp - 1,)),
                dma((n_tp - 1,)),
                dma((n_rep - 1,)),
                dma((n_rep - 1,)),
            ],
            compiler_params=pltpu.CompilerParams(
                collective_id=0, has_side_effects=True, vmem_limit_bytes=52 * 2**20
            ),
        )(layer_input, gate_saved, up_saved, out_grad, conv_taps, w_gate, w_up, w_down)
        grads, input_grad, taps = (pltpu.with_memory_space_constraint(v, pltpu.VMEM) for v in (grads, input_grad, taps))
        slots = min(4, hid // WIDE)
        return pl.pallas_call(
            widen,
            out_shape=(
                jax.ShapeDtypeStruct((seq, w), BF16),
                jax.ShapeDtypeStruct((dw, hid), F32),
                jax.ShapeDtypeStruct((dw, hid), F32),
                jax.ShapeDtypeStruct((hid, dw), F32),
                jax.ShapeDtypeStruct((3, hid), F32),
            ),
            in_specs=[vmem] * 3,
            out_specs=[any_spec] * 5,
            scratch_shapes=[
                pltpu.VMEM((slots, WIDE, dw), F32),
                pltpu.VMEM((2 * slots, dw, WIDE), F32),
                dma((slots,)),
                dma((2 * slots,)),
                dma((2,)),
            ],
            compiler_params=pltpu.CompilerParams(vmem_limit_bytes=24 * 2**20),
        )(grads, input_grad, taps)

    return jax.shard_map(
        local,
        mesh=mesh,
        in_specs=(
            P("rep", ("fs", "tp")), P("rep", "tp"), P("rep", "tp"), P("rep", None),
            P(None, "tp"), P("fs", "tp"), P("fs", "tp"), P("tp", "fs"),
        ),
        out_specs=(P("rep", ("fs", "tp")), P("fs", "tp"), P("fs", "tp"), P("tp", "fs"), P(None, "tp")),
        check_vma=False,
    )
```

```python
import functools

import jax
import jax.numpy as jnp
from jax import lax
from jax.experimental import pallas as pl
from jax.experimental.pallas import tpu as pltpu
from jax.sharding import PartitionSpec as P

MESH = pl.DeviceIdType.MESH
F32 = jnp.float32
BF16 = jnp.bfloat16
CH = 128
SUB = 4
HALF = CH // SUB
LAG = 2
HOP = 3
WIDE = 128


def kernel(n_rep, n_fs, n_tp, x_in, gate_in, up_in, og_in, taps_in, wg_in, wu_in, wd_in,
           from_in, ig_out, taps_out,
           xb, gate, up, og, wt, wg, wu, wd, act, part, from_out, gp, upp, terms, terms_in, taps_own, taps_all,
           xs_sem, xr_sem, gl_sem, ul_sem, ld_sem, wl_sem, ws_sem, wr_sem,
           in_s, in_r, out_s, out_r, ts_sem, tr_sem, ps_sem, pr_sem):
    rep, fs, tp = lax.axis_index("rep"), lax.axis_index("fs"), lax.axis_index("tp")
    seq, hid = gate.shape
    dw = wd_in.shape[1]
    w = x_in.shape[1]
    nj = hid // CH
    half = n_rep // 2
    low = rep < half
    depth = jnp.where(low, rep, n_rep - 1 - rep)
    inward = jnp.where(low, rep + 1, rep - 1)
    outward = jnp.where(low, rep - 1, rep + 1)
    has_out = depth > 0
    outward = jnp.where(has_out, outward, inward)
    innermost = depth == half - 1
    lag = LAG + HOP * SUB * (half - 1 - depth)
    lead = min(4, nj)
    steps = 3 * nj
    ring = in_r.shape[0]
    rest_end = lead - 1 + 2 * (nj - lead) + lead
    turns = max(steps + -(-LAG // SUB) + HOP * (half - 1), rest_end + n_tp + 5)

    def rows(j):
        return pl.ds(pl.multiple_of(j * CH, CH), CH)

    def piece(i):
        return pl.ds(pl.multiple_of(i * HALF, HALF), HALF)

    def unit(i):
        v, h = lax.div(i, SUB), lax.rem(i, SUB)
        a = v - lead
        b = a - 3 * (nj - lead)
        m = lax.rem(a, 3)
        mid = a < 3 * (nj - lead)
        first = a < 0
        k = jnp.where(first, 0, jnp.where(mid, jnp.where(m == 2, 0, m + 1), 1 + lax.rem(b, 2)))
        j = jnp.where(first, v, jnp.where(
            mid, lax.div(a, 3) + jnp.where(m == 2, lead, 0), nj - lead + lax.div(b, 2)))
        return SUB * j + h, k

    def fs_peer(d):
        return lax.rem(fs + d, n_fs)

    def tp_peer(d):
        return lax.rem(tp + d, n_tp)

    def load_gate(p):
        c = slice(0, CH) if p == 0 else slice(CH, hid)
        return pltpu.make_async_copy(gate_in.at[:, c], gate.at[:, c], gl_sem.at[p])

    def load_up(p):
        c = slice(0, CH) if p == 0 else slice(CH, hid)
        return pltpu.make_async_copy(up_in.at[:, c], up.at[:, c], ul_sem.at[p])

    load_wd = pltpu.make_async_copy(wd_in, wd.at[fs], wl_sem.at[0])

    def send_wd(j, d):
        return pltpu.make_async_remote_copy(
            src_ref=wd_in.at[rows(j), :], dst_ref=wd.at[fs, rows(j), :],
            send_sem=ws_sem.at[d - 1], recv_sem=wr_sem.at[d - 1, j],
            device_id={"fs": fs_peer(d)}, device_id_type=MESH)

    def recv_wd(j, d):
        src = lax.rem(fs + n_fs - d, n_fs)
        return pltpu.make_async_remote_copy(
            src_ref=wd_in.at[rows(j), :], dst_ref=wd.at[src, rows(j), :],
            send_sem=ws_sem.at[d - 1], recv_sem=wr_sem.at[d - 1, j],
            device_id={"fs": fs_peer(d)}, device_id_type=MESH)

    def x_copy(d, slot):
        return pltpu.make_async_remote_copy(
            src_ref=x_in, dst_ref=xb.at[slot], send_sem=xs_sem.at[d - 1], recv_sem=xr_sem.at[d - 1],
            device_id={"tp": tp_peer(d)}, device_id_type=MESH)

    def term_copy(d):
        return pltpu.make_async_remote_copy(
            src_ref=terms.at[tp_peer(d)], dst_ref=terms_in.at[d - 1],
            send_sem=ts_sem.at[d - 1], recv_sem=tr_sem.at[d - 1],
            device_id={"tp": tp_peer(d)}, device_id_type=MESH)

    def taps_copy(d, slot):
        return pltpu.make_async_remote_copy(
            src_ref=taps_all.at[rep], dst_ref=taps_all.at[slot],
            send_sem=ps_sem.at[d - 1], recv_sem=pr_sem.at[d - 1],
            device_id={"rep": lax.rem(rep + d, n_rep)}, device_id_type=MESH)

    def in_copy(i, j, k, dst):
        return pltpu.make_async_remote_copy(
            src_ref=part.at[k, piece(j), :], dst_ref=dst.at[k, piece(j), :],
            send_sem=in_s.at[k], recv_sem=(in_r if dst is from_out else out_r).at[lax.rem(i, ring)],
            device_id={"rep": inward}, device_id_type=MESH)

    def out_copy(i, j, k):
        return pltpu.make_async_remote_copy(
            src_ref=from_in.at[k, piece(j), :], dst_ref=from_in.at[k, piece(j), :],
            send_sem=out_s.at[k], recv_sem=out_r.at[lax.rem(i, ring)],
            device_id={"rep": outward}, device_id_type=MESH)

    def og_copy(d):
        cols = pl.ds(pl.multiple_of(fs_peer(d) * dw, dw), dw)
        return pltpu.make_async_copy(og_in.at[:, cols], og.at[:, cols], ld_sem.at[4 + d])

    loads = [
        pltpu.make_async_copy(taps_in, wt, ld_sem.at[0]),
        pltpu.make_async_copy(wg_in, wg, ld_sem.at[1]),
        pltpu.make_async_copy(wu_in, wu, ld_sem.at[2]),
        pltpu.make_async_copy(x_in, xb.at[tp], ld_sem.at[3]),
    ]
    taps_own[...] = jnp.zeros_like(taps_own)
    load_gate(0).start()
    load_up(0).start()
    loads[0].start()
    og_copy(0).start()

    barrier = pltpu.get_barrier_semaphore()
    for axis, n, me in (("rep", n_rep, rep), ("fs", n_fs, fs), ("tp", n_tp, tp)):
        for d in range(1, n):
            pl.semaphore_signal(barrier, inc=1, device_id={axis: lax.rem(me + d, n)}, device_id_type=MESH)
    for d in range(1, n_fs):
        og_copy(d).start()

    pos = lax.broadcasted_iota(jnp.int32, (seq, CH), 0)

    def back(v, n):
        return jnp.where(pos >= n, pltpu.roll(v, n, 0), 0.0)

    def ahead(v, n):
        return jnp.where(pos < seq - n, pltpu.roll(v, seq - n, 0), 0.0)

    def conv(j):
        g = gate[:, rows(j)].astype(F32)
        t = wt[:, rows(j)].astype(F32)
        b1, b2 = back(g, 1), back(g, 2)
        return g, b1, b2, t, t[0:1] * b2 + t[1:2] * b1 + t[2:3] * g

    tdot = functools.partial(lax.dot_general, dimension_numbers=(((0,), (0,)), ((), ())),
                             preferred_element_type=F32)
    wdot = functools.partial(lax.dot_general, dimension_numbers=(((1,), (1,)), ((), ())),
                             preferred_element_type=F32)

    own = pl.ds(pl.multiple_of(fs * dw, dw), dw)

    def down_first(j):
        @pl.when(j == 1)
        def _():
            load_gate(1).wait()
            load_up(1).wait()
        co = conv(j)[4]
        act[...] = (co * jax.nn.sigmoid(co) * up[:, rows(j)].astype(F32)).astype(BF16)

    def down_second(j):
        part[0, rows(j), :] = tdot(act[...], og[:, own]).astype(BF16)

    def rest_first(j):
        @pl.when(j == 0)
        def _():
            load_wd.wait()
        for d in range(1, n_fs):
            recv_wd(j, d).wait_recv()
        ag = wdot(og[:, 0:dw], wd[0, rows(j), :])
        for f in range(1, n_fs):
            ag = ag + wdot(og[:, f * dw:(f + 1) * dw], wd[f, rows(j), :])
        g, b1, b2, t, co = conv(j)
        s = jax.nn.sigmoid(co)
        upp[:, rows(j)] = (ag * (co * s)).astype(BF16)
        cg = ag * up[:, rows(j)].astype(F32) * s * (1.0 + co * (1.0 - s))
        gp[:, rows(j)] = (t[0:1] * ahead(cg, 2) + t[1:2] * ahead(cg, 1) + t[2:3] * cg).astype(BF16)
        for k, v in enumerate((b2, b1, g)):
            taps_own[pl.ds(3 * j + k, 1), :] = jnp.sum(cg * v, axis=0, keepdims=True)

    def rest_second(j):
        @pl.when(j == 0)
        def _():
            loads[3].wait()
            for d in range(1, n_tp):
                x_copy(d, lax.rem(tp + n_tp - d, n_tp)).wait_recv()
        g_part, u_part = gp[:, rows(j)], upp[:, rows(j)]
        for b in range(n_tp):
            part[1, rows(j), b * w:(b + 1) * w] = tdot(g_part, xb[b]).astype(BF16)
            part[2, rows(j), b * w:(b + 1) * w] = tdot(u_part, xb[b]).astype(BF16)

    def term_half(d, h):
        if h == 0:
            @pl.when(d == 1)
            def _():
                taps_all[rep] = taps_own[...].astype(BF16)
                for p in range(1, n_rep):
                    taps_copy(p, rep).start()
                loads[1].wait()
                loads[2].wait()
        b = tp_peer(d)
        r = pl.ds(pl.multiple_of(b * w, w), w)
        t = pl.ds(h * (seq // 2), seq // 2)
        terms[b, t, :] = (wdot(gp[t, :], wg[r, :]) + wdot(upp[t, :], wu[r, :])).astype(BF16)
        if h == 1:
            @pl.when(d < n_tp)
            def _():
                term_copy(d).start()

    def finish():
        total = terms[tp].astype(F32)
        for d in range(1, n_tp):
            term_copy(d).wait_recv()
            total = total + terms_in[d - 1].astype(F32)
        ig_out[...] = total.astype(BF16)
        for d in range(1, n_rep):
            taps_copy(d, lax.rem(rep + n_rep - d, n_rep)).wait_recv()
        acc = taps_all[0].astype(F32)
        for i in range(1, n_rep):
            acc = acc + taps_all[i].astype(F32)
        taps_own[...] = acc
        for j in range(nj):
            taps_out[0:3, j * CH:(j + 1) * CH] = taps_own[3 * j:3 * j + 3, :]
        for d in range(1, n_tp):
            x_copy(d, tp).wait_send()
            term_copy(d).wait_send()
        for d in range(1, n_rep):
            taps_copy(d, rep).wait_send()
        for d in range(1, n_fs):
            pltpu.make_async_remote_copy(
                src_ref=wd_in, dst_ref=wd.at[fs], send_sem=ws_sem.at[d - 1], recv_sem=wr_sem.at[d - 1, 0],
                device_id={"fs": fs_peer(d)}, device_id_type=MESH).wait_send()

    def q_stage(i):
        j, k = unit(i)

        @pl.when(has_out)
        def _():
            in_copy(i, j, k, from_out).wait_recv()
            r = piece(j)
            part[k, r, :] = part[k, r, :] + from_out[k, r, :]

        @pl.when(innermost)
        def _():
            in_copy(i, j, k, from_in).start()

        @pl.when(jnp.logical_not(innermost))
        def _():
            in_copy(i, j, k, from_out).start()

    def s_stage(i):
        j, k = unit(i)
        out_copy(i, j, k).wait_recv()

        @pl.when(innermost)
        def _():
            r = piece(j)
            from_in[k, r, :] = part[k, r, :] + from_in[k, r, :]

        @pl.when(has_out)
        def _():
            out_copy(i, j, k).start()

    load_gate(1).start()
    load_up(1).start()
    loads[0].wait()
    load_gate(0).wait()
    load_up(0).wait()
    down_first(0)
    og_copy(0).wait()
    down_second(0)
    pl.semaphore_wait(barrier, n_rep + n_fs + n_tp - 3)

    @pl.when(jnp.logical_not(has_out))
    def _():
        for h in range(SUB):
            q_stage(jnp.int32(h))
    for d in range(1, n_tp):
        x_copy(d, tp).start()

    def weights(j, c):
        for d in range(1, n_fs):
            send_wd(j, d).start()
        return c
    load_wd.start()
    lax.fori_loop(0, nj, weights, 0)
    for load in loads[1:]:
        load.start()
    for d in range(1, n_fs):
        og_copy(d).wait()

    def step(v, c):
        a = v - (lead - 1)
        b = a - 2 * (nj - lead)
        early = a < 0
        mid = jnp.logical_and(a >= 0, b < 0)
        is_down = jnp.logical_or(early, jnp.logical_and(mid, lax.rem(a, 2) == 1))
        is_rest = jnp.logical_and(jnp.logical_not(is_down), b < lead)
        is_term = jnp.logical_and(b >= lead, b < lead + n_tp)
        down_j = jnp.where(early, v + 1, lead + lax.div(a, 2))
        rest_j = jnp.where(mid, lax.div(a, 2), nj - lead + b)
        for h in range(SUB):
            i = SUB * v + h

            @pl.when(jnp.logical_and(v < steps, jnp.logical_or(v > 0, has_out)))
            def _():
                q_stage(i)
            turn = {0: 0, SUB // 2: 1}.get(h)
            if turn is not None:
                @pl.when(is_down)
                def _():
                    (down_first, down_second)[turn](down_j)

                @pl.when(is_rest)
                def _():
                    (rest_first, rest_second)[turn](rest_j)

                @pl.when(is_term)
                def _():
                    term_half(b - lead + 1, turn)

            si = i - lag

            @pl.when(jnp.logical_and(si >= 0, si < SUB * steps))
            def _():
                s_stage(si)

        @pl.when(v == rest_end + n_tp + 4)
        def _():
            finish()
        return c
    lax.fori_loop(0, turns, step, 0)

    for k in range(3):
        pltpu.make_async_remote_copy(
            src_ref=part.at[k], dst_ref=from_out.at[k], send_sem=in_s.at[k], recv_sem=in_r.at[0],
            device_id={"rep": inward}, device_id_type=MESH).wait_send()

        @pl.when(has_out)
        def _():
            pltpu.make_async_remote_copy(
                src_ref=from_in.at[k], dst_ref=from_in.at[k], send_sem=out_s.at[k], recv_sem=out_r.at[0],
                device_id={"rep": outward}, device_id_type=MESH).wait_send()


def widen(grads, input_grad, taps, ig_out, gate_out, up_out, down_out, taps_out, ring, ring_t, d_sem, t_sem, s_sem):
    hid, dw = down_out.shape
    slots = ring.shape[0]
    small = [
        pltpu.make_async_copy(input_grad, ig_out, s_sem.at[0]),
        pltpu.make_async_copy(taps.at[0:3, :], taps_out, s_sem.at[1]),
    ]
    for copy in small:
        copy.start()

    def down(i, s):
        return pltpu.make_async_copy(ring.at[s], down_out.at[pl.ds(i * WIDE, WIDE), :], d_sem.at[s])

    def wide(out, i, s):
        return pltpu.make_async_copy(ring_t.at[s], out.at[:, pl.ds(i * WIDE, WIDE)], t_sem.at[s])

    n = hid // WIDE
    for i in range(n):
        r = slice(i * WIDE, (i + 1) * WIDE)
        s = i % slots
        if i >= slots:
            down(i - slots, s).wait()
            wide(gate_out, i - slots, 2 * s).wait()
            wide(up_out, i - slots, 2 * s + 1).wait()
        ring[s] = grads[0, r, :].astype(F32)
        down(i, s).start()
        ring_t[2 * s] = grads[1, r, :].astype(F32).T
        wide(gate_out, i, 2 * s).start()
        ring_t[2 * s + 1] = grads[2, r, :].astype(F32).T
        wide(up_out, i, 2 * s + 1).start()
    for i in range(max(n - slots, 0), n):
        s = i % slots
        down(i, s).wait()
        wide(gate_out, i, 2 * s).wait()
        wide(up_out, i, 2 * s + 1).wait()
    for copy in small:
        copy.wait()


def solution(mesh):
    n_rep, n_fs, n_tp = mesh.shape["rep"], mesh.shape["fs"], mesh.shape["tp"]

    def local(layer_input, gate_saved, up_saved, out_grad, conv_taps, w_gate, w_up, w_down):
        seq, w = layer_input.shape
        dw, hid = w_gate.shape
        width = out_grad.shape[1]
        nj = hid // CH
        ring = min(LAG + HOP * SUB * (n_rep // 2 - 1) + 2, 3 * SUB * nj)
        tap_rows = -(-3 * nj // 16) * 16
        any_spec = pl.BlockSpec(memory_space=pl.ANY)
        vmem = pl.BlockSpec(memory_space=pltpu.VMEM)
        dma = pltpu.SemaphoreType.DMA
        grads, input_grad, taps = pl.pallas_call(
            functools.partial(kernel, n_rep, n_fs, n_tp),
            out_shape=(
                pltpu.VMEM((3, hid, dw), BF16),
                pltpu.VMEM((seq, w), BF16),
                pltpu.VMEM((8, hid), F32),
            ),
            in_specs=[any_spec] * 8,
            out_specs=(vmem, vmem, vmem),
            scratch_shapes=[
                pltpu.VMEM((n_tp, seq, w), BF16),
                pltpu.VMEM((seq, hid), BF16),
                pltpu.VMEM((seq, hid), BF16),
                pltpu.VMEM((seq, width), BF16),
                pltpu.VMEM((3, hid), BF16),
                pltpu.VMEM((dw, hid), BF16),
                pltpu.VMEM((dw, hid), BF16),
                pltpu.VMEM((n_fs, hid, dw), BF16),
                pltpu.VMEM((seq, CH), BF16),
                pltpu.VMEM((3, hid, dw), BF16),
                pltpu.VMEM((3, hid, dw), BF16),
                pltpu.VMEM((seq, hid), BF16),
                pltpu.VMEM((seq, hid), BF16),
                pltpu.VMEM((n_tp, seq, w), BF16),
                pltpu.VMEM((n_tp - 1, seq, w), BF16),
                pltpu.VMEM((tap_rows, CH), F32),
                pltpu.VMEM((n_rep, tap_rows, CH), BF16),
                dma((n_tp - 1,)),
                dma((n_tp - 1,)),
                dma((2,)),
                dma((2,)),
                dma((4 + n_fs,)),
                dma((1,)),
                dma((n_fs - 1,)),
                dma((n_fs - 1, nj)),
                dma((3,)),
                dma((ring,)),
                dma((3,)),
                dma((ring,)),
                dma((n_tp - 1,)),
                dma((n_tp - 1,)),
                dma((n_rep - 1,)),
                dma((n_rep - 1,)),
            ],
            compiler_params=pltpu.CompilerParams(
                collective_id=0, has_side_effects=True, vmem_limit_bytes=52 * 2**20
            ),
        )(layer_input, gate_saved, up_saved, out_grad, conv_taps, w_gate, w_up, w_down)
        grads, input_grad, taps = (pltpu.with_memory_space_constraint(v, pltpu.VMEM) for v in (grads, input_grad, taps))
        slots = min(4, hid // WIDE)
        return pl.pallas_call(
            widen,
            out_shape=(
                jax.ShapeDtypeStruct((seq, w), BF16),
                jax.ShapeDtypeStruct((dw, hid), F32),
                jax.ShapeDtypeStruct((dw, hid), F32),
                jax.ShapeDtypeStruct((hid, dw), F32),
                jax.ShapeDtypeStruct((3, hid), F32),
            ),
            in_specs=[vmem] * 3,
            out_specs=[any_spec] * 5,
            scratch_shapes=[
                pltpu.VMEM((slots, WIDE, dw), F32),
                pltpu.VMEM((2 * slots, dw, WIDE), F32),
                dma((slots,)),
                dma((2 * slots,)),
                dma((2,)),
            ],
            compiler_params=pltpu.CompilerParams(vmem_limit_bytes=24 * 2**20),
        )(grads, input_grad, taps)

    return jax.shard_map(
        local,
        mesh=mesh,
        in_specs=(
            P("rep", ("fs", "tp")), P("rep", "tp"), P("rep", "tp"), P("rep", None),
            P(None, "tp"), P("fs", "tp"), P("fs", "tp"), P("tp", "fs"),
        ),
        out_specs=(P("rep", ("fs", "tp")), P("fs", "tp"), P("fs", "tp"), P("tp", "fs"), P(None, "tp")),
        check_vma=False,
    )
```
